32 devices in a mesh: st: 16 (over z, y, x), tp: 2 (over core).
Axes of the slice: x: 2, y: 2, z: 4, core: 2. Of those that a mesh axis runs over, the one named last changes fastest.
Arguments:
- hidden: bfloat16 [16384, 2048], P('st'), may hold values from -6 to 6
- norm_gain: float32 [2048], replicated, may hold values from 0.1 to 1.9
- store: bfloat16 [384, 64, 2048], P('st'), may hold values from -6 to 6
- store_gain: float32 [2048], replicated, may hold values from 0.1 to 1.9
- passage_ids: int32 [128, 4], P('st'), may hold values from 0 to 383, as said below
- w_pool: bfloat16 [2048, 1024], P(None, 'tp'), may hold values from -0.125 to 0.125
- pool_mix: bfloat16 [4, 256, 256], P('tp'), may hold values from -0.375 to 0.375
- w_branch: bfloat16 [1024, 2048], P('tp'), may hold values from -0.1875 to 0.1875
- w_query: bfloat16 [2048, 512], P(None, 'tp'), may hold values from -0.125 to 0.125
- w_key: bfloat16 [2048, 512], P(None, 'tp'), may hold values from -0.125 to 0.125
- w_value: bfloat16 [2048, 512], P(None, 'tp'), may hold values from -0.125 to 0.125
- sharpness: float32 [4], P('tp'), may hold values from 1 to 90
- w_out: bfloat16 [512, 2048], P('tp'), may hold values from -0.25 to 0.25
- w_gate: bfloat16 [2048, 2048], P(None, 'tp'), may hold values from -0.125 to 0.125
Outputs:
- mixed: bfloat16 [16384, 2048], P('st', 'tp')
The draws below stay inside these ranges and needn't reach their ends.
Inputs may be any that keep to these rules, and one draw needn't show every extreme that they name: `passage_ids`: passage p lies on index p // 24 of st. The ids of one sequence's blocks (aligned rows of 32 ids) name passages of at most 4 reads on any one holder, counted with repeats, and some sequence reaches 4 at some holder in every draw.
All inputs are finite; a program needn't handle non-finite values.
Results may differ from the reference program's by a relative error of at most 0.0095.
The reference program's roundings to bfloat16 on the way (of `normed`, `pool_in`, `pooled`, `pool_out`, `query`, `passage_normed`, `weights` and `read`) count: a program that leaves them out, or rounds other values in their place, can miss the bound.
Values may be sent and summed in bfloat16 or wider, within the bound.
A program may use at most 128 MiB of HBM per device.

```python
import jax
import jax.numpy as jnp
from jax import lax

D = 2048
GROUPS = 4
GROUP_DIM = 256
XHEADS = 4
HEAD_DIM = 128
BLOCK = 128
PER_BLOCK = 4
PLEN = 64
PASS_DEV = 24
TOK_DEV = 1024
POOL_WIDTH = 1024
XWIDTH = 512
TOKENS = 16384
BLOCKS = 128
REQ_DEV = 32
MOST = 4
PASSAGES = 384
N_ST = 16
N_TP = 2


def draw_passage_ids(key, part):
    keys = jax.random.split(jax.random.fold_in(key, 11), 5)
    slots = N_ST * MOST
    devices = jnp.arange(N_ST)[:, None]
    slot_owner = jnp.broadcast_to(jnp.arange(slots)[None, :] // MOST, (N_ST, slots))
    forced = (slot_owner == (devices - 1) % N_ST) | (slot_owner == (devices + N_ST // 2) % N_ST)
    noise = jax.random.randint(keys[0], (N_ST, slots), 0, 1 << 20)
    score = jnp.where(forced, 0, noise + 1) * slots + jnp.arange(slots)[None, :]
    order = jnp.argsort(score, axis=1)[:, :REQ_DEV]
    chosen = jnp.take_along_axis(slot_owner, order, axis=1)
    shuffle = jax.random.randint(keys[1], (N_ST, REQ_DEV), 0, 1 << 20) * REQ_DEV + jnp.arange(REQ_DEV)[None, :]
    owners = jnp.take_along_axis(chosen, jnp.argsort(shuffle, axis=1), axis=1)
    local = jnp.minimum(jax.random.randint(keys[2], (N_ST, REQ_DEV), 0, PASS_DEV), jax.random.randint(keys[3], (N_ST, REQ_DEV), 0, PASS_DEV))
    local = jnp.minimum(local, jax.random.randint(keys[4], (N_ST, REQ_DEV), 0, PASS_DEV))
    return (owners * PASS_DEV + local).reshape(BLOCKS, PER_BLOCK).astype(jnp.int32)


def draw_sharpness(key, part):
    spread = jax.random.uniform(jax.random.fold_in(key, 23), (XHEADS,), jnp.float32)
    return jnp.exp(jnp.log(1.0) + spread * (jnp.log(4.0) - jnp.log(1.0)))


def steps_of(key, extent, cuts, low, largest):
    level, own = 1.0, jax.random.fold_in(key, 6)
    for dim, blocks in cuts:
        draws = jnp.exp(jax.random.uniform(jax.random.fold_in(own, dim), (blocks,), jnp.float32, low / len(cuts), largest / len(cuts)))
        level = level * jnp.repeat(draws, extent[dim] // blocks).reshape([-1 if axis == dim else 1 for axis in range(len(extent))])
    return level


def scatter_about(rng, extent, scale, reach, cuts=(), held_as=jnp.bfloat16):
    drawn = scale * jax.random.normal(rng, extent, jnp.float32)
    if cuts:
        drawn = drawn * steps_of(rng, extent, cuts, -0.22, 0.18)
    return jnp.clip(drawn, -reach, reach).astype(held_as)


def setup_inputs(seed: int = 0) -> dict:
    streams_of = jax.random.split(jax.random.key(seed), 15)
    hidden = scatter_about(streams_of[0], (TOKENS, D), 1.0, 6.0, ((0, 16),))
    norm_gain = jnp.clip(1.0 + 0.18 * jax.random.normal(streams_of[1], (D,), jnp.float32), 0.1, 1.9)
    store = scatter_about(streams_of[2], (PASSAGES, PLEN, D), 1.0, 6.0, ((0, 16),))
    store_gain = jnp.clip(1.0 + 0.18 * jax.random.normal(streams_of[3], (D,), jnp.float32), 0.1, 1.9)
    passage_ids = draw_passage_ids(jax.random.fold_in(streams_of[14], 71), 0)
    w_pool = scatter_about(streams_of[5], (D, POOL_WIDTH), D ** -0.5, 0.125, ((1, 2),))
    pool_mix = scatter_about(streams_of[6], (GROUPS, GROUP_DIM, GROUP_DIM), GROUP_DIM ** -0.5, 0.375, ((0, 2),))
    w_branch = scatter_about(streams_of[7], (POOL_WIDTH, D), POOL_WIDTH ** -0.5, 0.1875, ((0, 2),))
    w_query = scatter_about(streams_of[8], (D, XWIDTH), D ** -0.5, 0.125, ((1, 2),))
    w_key = scatter_about(streams_of[9], (D, XWIDTH), D ** -0.5, 0.125, ((1, 2),))
    w_value = scatter_about(streams_of[10], (D, XWIDTH), D ** -0.5, 0.125, ((1, 2),))
    sharpness = draw_sharpness(jax.random.fold_in(streams_of[14], 71), 0)
    w_out = scatter_about(streams_of[12], (XWIDTH, D), XWIDTH ** -0.5, 0.25, ((0, 2),))
    w_gate = scatter_about(streams_of[13], (D, D), D ** -0.5, 0.125, ((1, 2),))
    return {"hidden": hidden, "norm_gain": norm_gain, "store": store, "store_gain": store_gain, "passage_ids": passage_ids, "w_pool": w_pool, "pool_mix": pool_mix, "w_branch": w_branch, "w_query": w_query, "w_key": w_key, "w_value": w_value, "sharpness": sharpness, "w_out": w_out, "w_gate": w_gate}


def rms_norm(values, gain):
    wide = values.astype(jnp.float32)
    scale = lax.rsqrt(lax.optimization_barrier(jnp.mean(wide * wide, axis=-1, keepdims=True)) + 1e-05)
    return wide * scale * gain

def split_sum(left, right, pieces):
    width = left.shape[1] // pieces
    total = jnp.zeros((left.shape[0], right.shape[1]), jnp.float32)
    for index in range(pieces):
        term = jnp.dot(left[:, index * width:(index + 1) * width], right[index * width:(index + 1) * width], preferred_element_type=jnp.float32).astype(jnp.bfloat16)
        term = lax.optimization_barrier(term)
        total = total + term.astype(jnp.float32)
    return total

def reference(hidden, norm_gain, store, store_gain, passage_ids, w_pool, pool_mix, w_branch, w_query, w_key, w_value, sharpness, w_out, w_gate):
    normed = rms_norm(hidden, norm_gain).astype(jnp.bfloat16)
    pool_in = jnp.dot(normed, w_pool, preferred_element_type=jnp.float32).astype(jnp.bfloat16)
    grouped = pool_in.astype(jnp.float32).reshape(N_ST, TOK_DEV, GROUPS, GROUP_DIM)
    position = jnp.arange(TOK_DEV)
    outputs = []
    for group in range(GROUPS):
        window = 2 ** (group + 1)
        column = grouped[:, :, group]
        total = jnp.zeros_like(column)
        for shift in range(window):
            total = total + jnp.pad(column, ((0, 0), (shift, 0), (0, 0)))[:, :TOK_DEV]
        count = jnp.minimum(position + 1, window).astype(jnp.float32)[None, :, None]
        outputs.append(total / count - column)
    pooled = jnp.stack(outputs, axis=2).astype(jnp.bfloat16)
    pool_out = jnp.einsum('ntgc,gcd->ntgd', pooled.astype(jnp.float32), pool_mix.astype(jnp.float32))
    pool_out = pool_out.astype(jnp.bfloat16).reshape(TOKENS, POOL_WIDTH)
    branch_pool = split_sum(pool_out, w_branch, N_TP)
    query = jnp.dot(normed, w_query, preferred_element_type=jnp.float32).astype(jnp.bfloat16)
    query_blocks = query.reshape(BLOCKS, BLOCK, XHEADS, HEAD_DIM)
    scale = sharpness / HEAD_DIM ** 0.5

    def one_block(items):
        block_query, ids = items
        rows = store[ids].reshape(PER_BLOCK * PLEN, D)
        passage_normed = rms_norm(rows, store_gain).astype(jnp.bfloat16)
        keys = jnp.dot(passage_normed, w_key, preferred_element_type=jnp.float32).astype(jnp.bfloat16)
        values = jnp.dot(passage_normed, w_value, preferred_element_type=jnp.float32).astype(jnp.bfloat16)
        keys = keys.reshape(PER_BLOCK * PLEN, XHEADS, HEAD_DIM).astype(jnp.float32)
        values = values.reshape(PER_BLOCK * PLEN, XHEADS, HEAD_DIM).astype(jnp.float32)
        scores = jnp.einsum('qhd,khd->hqk', block_query.astype(jnp.float32), keys) * scale[:, None, None]
        weights = jax.nn.softmax(scores, axis=-1).astype(jnp.bfloat16)
        read = jnp.einsum('hqk,khd->qhd', weights.astype(jnp.float32), values)
        return read.astype(jnp.bfloat16).reshape(BLOCK, XWIDTH)
    read = lax.map(one_block, (query_blocks, passage_ids)).reshape(TOKENS, XWIDTH)
    branch_read = split_sum(read, w_out, N_TP)
    gate = jax.nn.sigmoid(jnp.dot(normed, w_gate, preferred_element_type=jnp.float32))
    return (branch_pool + gate * branch_read).astype(jnp.bfloat16)
```

```python
import functools
import math

import jax
import jax.numpy as jnp
from jax import lax
from jax.experimental import pallas as pl
from jax.experimental.pallas import tpu as pltpu
from jax.sharding import PartitionSpec as P

GROUPS = 4
PLANES = 4
RELAY = True


def rms_norm(values, gain):
    wide = values.astype(jnp.float32)
    scale = lax.rsqrt(jnp.mean(wide * wide, axis=-1, keepdims=True) + 1e-05)
    return wide * scale * gain


def pool_branch(normed, w_pool, pool_mix):
    tokens = normed.shape[0]
    local_groups = pool_mix.shape[0]
    group_dim = pool_mix.shape[1]
    pool_in = jnp.dot(normed, w_pool, preferred_element_type=jnp.float32).astype(jnp.bfloat16)
    grouped = pool_in.astype(jnp.float32).reshape(tokens, local_groups, group_dim)
    group_index = lax.axis_index("tp") * local_groups + jnp.arange(local_groups, dtype=jnp.int32)
    window = jnp.power(2, group_index + 1)
    total = jnp.zeros_like(grouped)
    for shift in range(2**GROUPS):
        shifted = jnp.pad(grouped, ((shift, 0), (0, 0), (0, 0)))[:tokens]
        total = total + jnp.where(shift < window, 1.0, 0.0)[None, :, None] * shifted
    position = jnp.arange(tokens, dtype=jnp.int32)[:, None]
    count = jnp.minimum(position + 1, window[None, :]).astype(jnp.float32)
    pooled = (total / count[:, :, None] - grouped).astype(jnp.bfloat16)
    pool_out = jnp.einsum("tgc,gcd->tgd", pooled, pool_mix, preferred_element_type=jnp.float32)
    return pool_out.astype(jnp.bfloat16).reshape(tokens, local_groups * group_dim)


def half_terms(own, other, weight_own, weight_other):
    terms = [
        jnp.dot(a, w, preferred_element_type=jnp.float32).astype(jnp.bfloat16).astype(jnp.float32)
        for a, w in ((own, weight_own), (other, weight_other))
    ]
    return terms[0] + terms[1]


def swap(array):
    return lax.ppermute(array, "tp", [(0, 1), (1, 0)])


def columns_of(weight, part):
    half = weight.shape[1] // 2
    return lax.dynamic_slice_in_dim(weight, part * half, half, axis=1)


class Exchange:
    def __init__(self, n):
        self.n = n
        self.planes = PLANES if n % PLANES == 0 and n > PLANES else 1
        self.q = n // self.planes
        self.xor = self.q & (self.q - 1) == 0
        self.steps = [(dz, dp) for dz in range(self.planes) for dp in range(self.q)]

    def to(self, me, dz, dp):
        z, p = me // self.q, me % self.q
        side = (p ^ dp) if self.xor else (p + dp) % self.q
        return ((z + dz) % self.planes) * self.q + side

    def step_of(self, me, source):
        dz = (me // self.q - source // self.q) % self.planes
        dp = (me % self.q) ^ (source % self.q) if self.xor else (me % self.q - source % self.q) % self.q
        return dz * self.q + dp

    def move(self, block, dz, dp):
        return lax.ppermute(block, "st", [(i, self.to(i, dz, dp)) for i in range(self.n)])

    def run(self, blocks):
        arrived = [None] * self.n
        arrived[0] = blocks[0]
        opposite = self.planes // 2
        split = RELAY and self.planes == 4
        half = blocks[0].shape[0] // 2
        if split:
            far = range(opposite * self.q, (opposite + 1) * self.q)
            bundle = self.move(jnp.concatenate([blocks[s][half:] for s in far], axis=0), self.planes - 1, 0)
        order = sorted(range(1, self.n), key=lambda s: (abs(self.steps[s][0] - opposite), s))
        for s in order:
            dz, dp = self.steps[s]
            if split and dz == opposite:
                first = self.move(blocks[s][:half], dz, dp)
                last = self.move(bundle[dp * half : (dp + 1) * half], self.planes - 1, dp)
                arrived[s] = jnp.concatenate([first, last], axis=0)
            else:
                arrived[s] = self.move(blocks[s], dz, dp)
        return jnp.concatenate(arrived, axis=0)


def attention_kernel(heads, slots_ref, scale_ref, q_ref, *refs):
    parts, out_ref = refs[:-1], refs[-1]
    kv = jnp.concatenate([r[0] for r in parts], axis=0)
    width = q_ref.shape[1]
    head_dim = width // heads
    for h in range(heads):
        cut = slice(h * head_dim, (h + 1) * head_dim)
        scores = lax.dot_general(
            q_ref[:, cut], kv[:, cut], (((1,), (1,)), ((), ())), preferred_element_type=jnp.float32
        )
        scores = scores * scale_ref[h]
        top = jnp.exp(scores - jnp.max(scores, axis=-1, keepdims=True))
        weights = (top / jnp.sum(top, axis=-1, keepdims=True)).astype(jnp.bfloat16)
        out_ref[:, cut] = jnp.dot(
            weights, kv[:, width + h * head_dim : width + (h + 1) * head_dim],
            preferred_element_type=jnp.float32,
        ).astype(jnp.bfloat16)


def attend(query, kv, block_slot, scale):
    blocks_dev, per_block = block_slot.shape
    tokens, width = query.shape
    block_len = tokens // blocks_dev
    length, both = kv.shape[1:]
    heads = scale.shape[0]

    def part(j):
        return pl.BlockSpec((1, length, both), lambda b, slots: (slots[b * per_block + j], 0, 0))

    return pl.pallas_call(
        functools.partial(attention_kernel, heads),
        out_shape=jax.ShapeDtypeStruct((tokens, width), jnp.bfloat16),
        grid_spec=pltpu.PrefetchScalarGridSpec(
            num_scalar_prefetch=1,
            grid=(blocks_dev,),
            in_specs=[
                pl.BlockSpec(memory_space=pltpu.SMEM),
                pl.BlockSpec((block_len, width), lambda b, slots: (b, 0)),
            ] + [part(j) for j in range(per_block)],
            out_specs=pl.BlockSpec((block_len, width), lambda b, slots: (b, 0)),
        ),
        cost_estimate=pl.CostEstimate(
            flops=4 * tokens * per_block * length * width, bytes_accessed=4 * 2**20, transcendentals=0
        ),
    )(block_slot.reshape(-1), scale, query, *([kv] * per_block))


def body(
    hidden,
    norm_gain,
    store,
    store_gain,
    passage_ids,
    w_pool,
    pool_mix,
    w_branch,
    w_query,
    w_key,
    w_value,
    sharpness,
    w_out,
    w_gate,
):
    holders = lax.axis_size("st")
    me = lax.axis_index("st")
    core = lax.axis_index("tp")
    flat_ids = passage_ids.reshape(-1)
    reads = flat_ids.shape[0]
    pass_dev, length, width = store.shape
    exchange = Exchange(holders)
    owner = flat_ids // pass_dev
    local = flat_ids % pass_dev
    order = jnp.arange(reads, dtype=jnp.int32)
    earlier = (owner[None, :] == owner[:, None]) & (order[None, :] < order[:, None])
    rank = jnp.sum(earlier.astype(jnp.int32), axis=1)
    most = max(1, 2 * reads // holders)
    wanted = owner * most + rank
    hits = wanted[None, :] == jnp.arange(holders * most, dtype=jnp.int32)[:, None]
    request = jnp.sum(jnp.where(hits, local[None, :], 0), axis=1).reshape(holders, most)
    incoming = lax.all_to_all(request, "st", split_axis=0, concat_axis=0, tiled=True)

    passage_normed = rms_norm(store, store_gain).astype(jnp.bfloat16).reshape(pass_dev * length, width)
    w_kv = jnp.concatenate([w_key, w_value], axis=1)
    own_kv = jnp.dot(passage_normed, w_kv, preferred_element_type=jnp.float32).astype(jnp.bfloat16)
    own_kv = own_kv.reshape(pass_dev, length, -1)
    peers = jnp.stack([exchange.to(me, dz, dp) for dz, dp in exchange.steps])
    chosen = incoming[peers]
    blocks = [own_kv[chosen[s]].reshape(most * length, -1) for s in range(holders)]
    kv = exchange.run(blocks).reshape(holders * most, length, -1)
    slot = exchange.step_of(me, owner) * most + rank

    w_out_other = swap(columns_of(w_out, 1 - core))
    w_branch_other = swap(columns_of(w_branch, 1 - core))
    normed = rms_norm(hidden, norm_gain).astype(jnp.bfloat16)
    pool_out = pool_branch(normed, w_pool, pool_mix)
    branch_pool = half_terms(pool_out, swap(pool_out), columns_of(w_branch, core), w_branch_other)
    gate = jax.nn.sigmoid(jnp.dot(normed, w_gate, preferred_element_type=jnp.float32))
    query = jnp.dot(normed, w_query, preferred_element_type=jnp.float32).astype(jnp.bfloat16)

    head_dim = query.shape[1] // sharpness.shape[0]
    read = attend(query, kv, slot.reshape(passage_ids.shape), sharpness / math.sqrt(head_dim))
    branch_read = half_terms(read, swap(read), columns_of(w_out, core), w_out_other)
    return (branch_pool + gate * branch_read).astype(jnp.bfloat16)


def solution(mesh):
    placed = (
        P("st", None),
        P(),
        P("st", None, None),
        P(),
        P("st", None),
        P(None, "tp"),
        P("tp", None, None),
        P("tp", None),
        P(None, "tp"),
        P(None, "tp"),
        P(None, "tp"),
        P("tp"),
        P("tp", None),
        P(None, "tp"),
    )
    return jax.shard_map(body, mesh=mesh, in_specs=placed, out_specs=P("st", "tp"), check_vma=False)
```

```python
import functools
import math

import jax
import jax.numpy as jnp
from jax import lax
from jax.experimental import pallas as pl
from jax.experimental.pallas import tpu as pltpu
from jax.sharding import PartitionSpec as P

GROUPS = 4


def rms_norm(values, gain):
    wide = values.astype(jnp.float32)
    scale = lax.rsqrt(jnp.mean(wide * wide, axis=-1, keepdims=True) + 1e-05)
    return wide * scale * gain


def pool_branch(normed, w_pool, pool_mix):
    tokens = normed.shape[0]
    local_groups = pool_mix.shape[0]
    group_dim = pool_mix.shape[1]
    pool_in = jnp.dot(normed, w_pool, preferred_element_type=jnp.float32).astype(jnp.bfloat16)
    grouped = pool_in.astype(jnp.float32).reshape(tokens, local_groups, group_dim)
    group_index = lax.axis_index("tp") * local_groups + jnp.arange(local_groups, dtype=jnp.int32)
    window = jnp.power(2, group_index + 1)
    total = jnp.zeros_like(grouped)
    for shift in range(2**GROUPS):
        shifted = jnp.pad(grouped, ((shift, 0), (0, 0), (0, 0)))[:tokens]
        total = total + jnp.where(shift < window, 1.0, 0.0)[None, :, None] * shifted
    position = jnp.arange(tokens, dtype=jnp.int32)[:, None]
    count = jnp.minimum(position + 1, window[None, :]).astype(jnp.float32)
    pooled = (total / count[:, :, None] - grouped).astype(jnp.bfloat16)
    pool_out = jnp.einsum("tgc,gcd->tgd", pooled, pool_mix, preferred_element_type=jnp.float32)
    return pool_out.astype(jnp.bfloat16).reshape(tokens, local_groups * group_dim)


def half_terms(own, other, weight_own, weight_other):
    terms = [
        jnp.dot(a, w, preferred_element_type=jnp.float32).astype(jnp.bfloat16).astype(jnp.float32)
        for a, w in ((own, weight_own), (other, weight_other))
    ]
    return terms[0] + terms[1]


def swap(array):
    return lax.ppermute(array, "tp", [(0, 1), (1, 0)])


def columns_of(weight, part):
    half = weight.shape[1] // 2
    return lax.dynamic_slice_in_dim(weight, part * half, half, axis=1)


def attention_kernel(heads, slots_ref, scale_ref, q_ref, *refs):
    parts, out_ref = refs[:-1], refs[-1]
    kv = jnp.concatenate([r[0] for r in parts], axis=0)
    width = q_ref.shape[1]
    head_dim = width // heads
    for h in range(heads):
        cut = slice(h * head_dim, (h + 1) * head_dim)
        scores = lax.dot_general(
            q_ref[:, cut], kv[:, cut], (((1,), (1,)), ((), ())), preferred_element_type=jnp.float32
        )
        scores = scores * scale_ref[h]
        top = jnp.exp(scores - jnp.max(scores, axis=-1, keepdims=True))
        weights = (top / jnp.sum(top, axis=-1, keepdims=True)).astype(jnp.bfloat16)
        out_ref[:, cut] = jnp.dot(
            weights, kv[:, width + h * head_dim : width + (h + 1) * head_dim],
            preferred_element_type=jnp.float32,
        ).astype(jnp.bfloat16)


def attend(query, kv, block_slot, scale):
    blocks_dev, per_block = block_slot.shape
    tokens, width = query.shape
    block_len = tokens // blocks_dev
    length, both = kv.shape[1:]
    heads = scale.shape[0]

    def part(j):
        return pl.BlockSpec((1, length, both), lambda b, slots: (slots[b * per_block + j], 0, 0))

    return pl.pallas_call(
        functools.partial(attention_kernel, heads),
        out_shape=jax.ShapeDtypeStruct((tokens, width), jnp.bfloat16),
        grid_spec=pltpu.PrefetchScalarGridSpec(
            num_scalar_prefetch=1,
            grid=(blocks_dev,),
            in_specs=[
                pl.BlockSpec(memory_space=pltpu.SMEM),
                pl.BlockSpec((block_len, width), lambda b, slots: (b, 0)),
            ] + [part(j) for j in range(per_block)],
            out_specs=pl.BlockSpec((block_len, width), lambda b, slots: (b, 0)),
        ),
        cost_estimate=pl.CostEstimate(
            flops=4 * tokens * per_block * length * width, bytes_accessed=4 * 2**20, transcendentals=0
        ),
    )(block_slot.reshape(-1), scale, query, *([kv] * per_block))


def body(
    hidden,
    norm_gain,
    store,
    store_gain,
    passage_ids,
    w_pool,
    pool_mix,
    w_branch,
    w_query,
    w_key,
    w_value,
    sharpness,
    w_out,
    w_gate,
):
    holders = lax.axis_size("st")
    core = lax.axis_index("tp")
    flat_ids = passage_ids.reshape(-1)
    reads = flat_ids.shape[0]
    pass_dev, length, width = store.shape
    owner = flat_ids // pass_dev
    local = flat_ids % pass_dev
    order = jnp.arange(reads, dtype=jnp.int32)
    earlier = (owner[None, :] == owner[:, None]) & (order[None, :] < order[:, None])
    rank = jnp.sum(earlier.astype(jnp.int32), axis=1)
    most = max(1, 2 * reads // holders)
    wanted = owner * most + rank
    hits = wanted[None, :] == jnp.arange(holders * most, dtype=jnp.int32)[:, None]
    request = jnp.sum(jnp.where(hits, local[None, :], 0), axis=1).reshape(holders, most)
    incoming = lax.all_to_all(request, "st", split_axis=0, concat_axis=0, tiled=True)

    passage_normed = rms_norm(store, store_gain).astype(jnp.bfloat16).reshape(pass_dev * length, width)
    w_kv = jnp.concatenate([w_key, w_value], axis=1)
    own_kv = jnp.dot(passage_normed, w_kv, preferred_element_type=jnp.float32).astype(jnp.bfloat16)
    own_kv = own_kv.reshape(pass_dev, length, -1)
    packed = own_kv[incoming.reshape(-1)]
    packed, hidden, w_out, w_branch = lax.optimization_barrier((packed, hidden, w_out, w_branch))
    kv = lax.all_to_all(packed, "st", split_axis=0, concat_axis=0, tiled=True)
    slot = wanted

    w_out_other = swap(columns_of(w_out, 1 - core))
    w_branch_other = swap(columns_of(w_branch, 1 - core))
    normed = rms_norm(hidden, norm_gain).astype(jnp.bfloat16)
    pool_out = pool_branch(normed, w_pool, pool_mix)
    branch_pool = half_terms(pool_out, swap(pool_out), columns_of(w_branch, core), w_branch_other)
    gate = jax.nn.sigmoid(jnp.dot(normed, w_gate, preferred_element_type=jnp.float32))
    query = jnp.dot(normed, w_query, preferred_element_type=jnp.float32).astype(jnp.bfloat16)

    head_dim = query.shape[1] // sharpness.shape[0]
    read = attend(query, kv, slot.reshape(passage_ids.shape), sharpness / math.sqrt(head_dim))
    branch_read = half_terms(read, swap(read), columns_of(w_out, core), w_out_other)
    return (branch_pool + gate * branch_read).astype(jnp.bfloat16)


def solution(mesh):
    placed = (
        P("st", None),
        P(),
        P("st", None, None),
        P(),
        P("st", None),
        P(None, "tp"),
        P("tp", None, None),
        P("tp", None),
        P(None, "tp"),
        P(None, "tp"),
        P(None, "tp"),
        P("tp"),
        P("tp", None),
        P(None, "tp"),
    )
    return jax.shard_map(body, mesh=mesh, in_specs=placed, out_specs=P("st", "tp"), check_vma=False)
```

```python
import functools
import math

import jax
import jax.numpy as jnp
from jax import lax
from jax.experimental import pallas as pl
from jax.experimental.pallas import tpu as pltpu
from jax.sharding import PartitionSpec as P

GROUPS = 4
ATTEND_BLOCKS = 2
MESH = pl.DeviceIdType.MESH


def rms_norm(values, gain):
    wide = values.astype(jnp.float32)
    scale = lax.rsqrt(jnp.mean(wide * wide, axis=-1, keepdims=True) + 1e-05)
    return wide * scale * gain


def pool_branch(normed, w_pool, pool_mix):
    tokens = normed.shape[0]
    local_groups = pool_mix.shape[0]
    group_dim = pool_mix.shape[1]
    pool_in = jnp.dot(normed, w_pool, preferred_element_type=jnp.float32).astype(jnp.bfloat16)
    grouped = pool_in.astype(jnp.float32).reshape(tokens, local_groups, group_dim)
    group_index = lax.axis_index("tp") * local_groups + jnp.arange(local_groups, dtype=jnp.int32)
    window = jnp.power(2, group_index + 1)
    total = jnp.zeros_like(grouped)
    for shift in range(2**GROUPS):
        shifted = jnp.pad(grouped, ((shift, 0), (0, 0), (0, 0)))[:tokens]
        total = total + jnp.where(shift < window, 1.0, 0.0)[None, :, None] * shifted
    position = jnp.arange(tokens, dtype=jnp.int32)[:, None]
    count = jnp.minimum(position + 1, window[None, :]).astype(jnp.float32)
    pooled = (total / count[:, :, None] - grouped).astype(jnp.bfloat16)
    pool_out = jnp.einsum("tgc,gcd->tgd", pooled, pool_mix, preferred_element_type=jnp.float32)
    return pool_out.astype(jnp.bfloat16).reshape(tokens, local_groups * group_dim)


def half_terms(own, other, weight_own, weight_other):
    terms = [
        jnp.dot(a, w, preferred_element_type=jnp.float32).astype(jnp.bfloat16).astype(jnp.float32)
        for a, w in ((own, weight_own), (other, weight_other))
    ]
    return terms[0] + terms[1]


def swap(array):
    return lax.ppermute(array, "tp", [(0, 1), (1, 0)])


def columns_of(weight, part):
    half = weight.shape[1] // 2
    return lax.dynamic_slice_in_dim(weight, part * half, half, axis=1)


def attention_kernel(heads, group, slots_ref, scale_ref, q_ref, *refs):
    parts, out_ref = refs[:-1], refs[-1]
    width = q_ref.shape[1]
    head_dim = width // heads
    block_len = q_ref.shape[0] // group
    per_block = len(parts) // group
    for b, h in [(b, h) for b in range(group) for h in range(heads)]:
        rows = slice(b * block_len, (b + 1) * block_len)
        kv = jnp.concatenate([r[0] for r in parts[b * per_block : (b + 1) * per_block]], axis=0)
        cut = slice(h * head_dim, (h + 1) * head_dim)
        scores = lax.dot_general(
            q_ref[rows, cut], kv[:, cut], (((1,), (1,)), ((), ())), preferred_element_type=jnp.float32
        )
        scores = scores * scale_ref[h]
        top = jnp.exp(scores - jnp.max(scores, axis=-1, keepdims=True))
        weights = (top * (1.0 / jnp.sum(top, axis=-1, keepdims=True))).astype(jnp.bfloat16)
        out_ref[rows, cut] = jnp.dot(
            weights, kv[:, width + h * head_dim : width + (h + 1) * head_dim],
            preferred_element_type=jnp.float32,
        ).astype(jnp.bfloat16)


def attend(query, kv, block_slot, scale):
    blocks_dev, per_block = block_slot.shape
    tokens, width = query.shape
    block_len = tokens // blocks_dev
    length, both = kv.shape[1:]
    heads = scale.shape[0]
    group = math.gcd(blocks_dev, ATTEND_BLOCKS)
    taken = group * per_block

    def part(j):
        return pl.BlockSpec((1, length, both), lambda b, slots: (slots[b * taken + j], 0, 0))

    return pl.pallas_call(
        functools.partial(attention_kernel, heads, group),
        out_shape=jax.ShapeDtypeStruct((tokens, width), jnp.bfloat16),
        grid_spec=pltpu.PrefetchScalarGridSpec(
            num_scalar_prefetch=1,
            grid=(blocks_dev // group,),
            in_specs=[
                pl.BlockSpec(memory_space=pltpu.SMEM),
                pl.BlockSpec((group * block_len, width), lambda b, slots: (b, 0)),
            ] + [part(j) for j in range(taken)],
            out_specs=pl.BlockSpec((group * block_len, width), lambda b, slots: (b, 0)),
        ),
        cost_estimate=pl.CostEstimate(
            flops=4 * tokens * per_block * length * width, bytes_accessed=4 * 2**20, transcendentals=0
        ),
    )(block_slot.reshape(-1), scale, query, *([kv] * taken))


def body(
    hidden,
    norm_gain,
    store,
    store_gain,
    passage_ids,
    w_pool,
    pool_mix,
    w_branch,
    w_query,
    w_key,
    w_value,
    sharpness,
    w_out,
    w_gate,
):
    holders = lax.axis_size("st")
    core = lax.axis_index("tp")
    flat_ids = passage_ids.reshape(-1)
    reads = flat_ids.shape[0]
    pass_dev, length, width = store.shape
    owner = lax.div(flat_ids, pass_dev)
    local = flat_ids - owner * pass_dev
    order = jnp.arange(reads, dtype=jnp.int32)
    earlier = (owner[None, :] == owner[:, None]) & (order[None, :] < order[:, None])
    rank = jnp.sum(earlier.astype(jnp.int32), axis=1)
    most = max(1, 2 * reads // holders)
    wanted = owner * most + rank
    hits = wanted[None, :] == jnp.arange(holders * most, dtype=jnp.int32)[:, None]
    request = jnp.sum(jnp.where(hits, local[None, :], 0), axis=1).reshape(holders, most)
    incoming = lax.all_to_all(request, "st", split_axis=0, concat_axis=0, tiled=True)

    passage_normed = rms_norm(store, store_gain).astype(jnp.bfloat16).reshape(pass_dev * length, width)
    w_kv = jnp.concatenate([w_key, w_value], axis=1)
    own_kv = jnp.dot(passage_normed, w_kv, preferred_element_type=jnp.float32).astype(jnp.bfloat16)
    own_kv = own_kv.reshape(pass_dev, length, -1)
    packed = own_kv[incoming.reshape(-1)]
    packed, hidden, w_out, w_branch = lax.optimization_barrier((packed, hidden, w_out, w_branch))
    kv = lax.all_to_all(packed, "st", split_axis=0, concat_axis=0, tiled=True)
    slot = wanted

    w_out_other = swap(columns_of(w_out, 1 - core))
    w_branch_other = swap(columns_of(w_branch, 1 - core))
    normed = rms_norm(hidden, norm_gain).astype(jnp.bfloat16)
    pool_out = pool_branch(normed, w_pool, pool_mix)
    branch_pool = half_terms(pool_out, swap(pool_out), columns_of(w_branch, core), w_branch_other)
    gate = jax.nn.sigmoid(jnp.dot(normed, w_gate, preferred_element_type=jnp.float32))
    query = jnp.dot(normed, w_query, preferred_element_type=jnp.float32).astype(jnp.bfloat16)

    head_dim = query.shape[1] // sharpness.shape[0]
    read = attend(query, kv, slot.reshape(passage_ids.shape), sharpness / math.sqrt(head_dim))
    branch_read = half_terms(read, swap(read), columns_of(w_out, core), w_out_other)
    return (branch_pool + gate * branch_read).astype(jnp.bfloat16)


def solution(mesh):
    placed = (
        P("st", None),
        P(),
        P("st", None, None),
        P(),
        P("st", None),
        P(None, "tp"),
        P("tp", None, None),
        P("tp", None),
        P(None, "tp"),
        P(None, "tp"),
        P(None, "tp"),
        P("tp"),
        P("tp", None),
        P(None, "tp"),
    )
    return jax.shard_map(body, mesh=mesh, in_specs=placed, out_specs=P("st", "tp"), check_vma=False)
```

```python
import functools
import math

import jax
import jax.numpy as jnp
from jax import lax
from jax.experimental import pallas as pl
from jax.experimental.pallas import tpu as pltpu
from jax.sharding import PartitionSpec as P

GROUPS = 4
ATTEND_BLOCKS = 4
MESH = pl.DeviceIdType.MESH


def rms_norm(values, gain):
    wide = values.astype(jnp.float32)
    scale = lax.rsqrt(jnp.mean(wide * wide, axis=-1, keepdims=True) + 1e-05)
    return wide * scale * gain


def pool_branch(normed, w_pool, pool_mix):
    tokens = normed.shape[0]
    local_groups = pool_mix.shape[0]
    group_dim = pool_mix.shape[1]
    pool_in = jnp.dot(normed, w_pool, preferred_element_type=jnp.float32).astype(jnp.bfloat16)
    grouped = pool_in.astype(jnp.float32).reshape(tokens, local_groups, group_dim)
    group_index = lax.axis_index("tp") * local_groups + jnp.arange(local_groups, dtype=jnp.int32)
    window = jnp.power(2, group_index + 1)
    total = jnp.zeros_like(grouped)
    for shift in range(2**GROUPS):
        shifted = jnp.pad(grouped, ((shift, 0), (0, 0), (0, 0)))[:tokens]
        total = total + jnp.where(shift < window, 1.0, 0.0)[None, :, None] * shifted
    position = jnp.arange(tokens, dtype=jnp.int32)[:, None]
    count = jnp.minimum(position + 1, window[None, :]).astype(jnp.float32)
    pooled = (total / count[:, :, None] - grouped).astype(jnp.bfloat16)
    pool_out = jnp.einsum("tgc,gcd->tgd", pooled, pool_mix, preferred_element_type=jnp.float32)
    return pool_out.astype(jnp.bfloat16).reshape(tokens, local_groups * group_dim)


def half_terms(own, other, weight_own, weight_other):
    terms = [
        jnp.dot(a, w, preferred_element_type=jnp.float32).astype(jnp.bfloat16).astype(jnp.float32)
        for a, w in ((own, weight_own), (other, weight_other))
    ]
    return terms[0] + terms[1]


def swap(array):
    return lax.ppermute(array, "tp", [(0, 1), (1, 0)])


def columns_of(weight, part):
    half = weight.shape[1] // 2
    return lax.dynamic_slice_in_dim(weight, part * half, half, axis=1)


def attention_kernel(heads, group, slots_ref, scale_ref, q_ref, *refs):
    parts, out_ref = refs[:-1], refs[-1]
    width = q_ref.shape[1]
    head_dim = width // heads
    block_len = q_ref.shape[0] // group
    per_block = len(parts) // group
    for b, h in [(b, h) for b in range(group) for h in range(heads)]:
        rows = slice(b * block_len, (b + 1) * block_len)
        kv = jnp.concatenate([r[0] for r in parts[b * per_block : (b + 1) * per_block]], axis=0)
        cut = slice(h * head_dim, (h + 1) * head_dim)
        scores = lax.dot_general(
            q_ref[rows, cut], kv[:, cut], (((1,), (1,)), ((), ())), preferred_element_type=jnp.float32
        )
        scores = scores * scale_ref[h]
        top = jnp.exp(scores - jnp.max(scores, axis=-1, keepdims=True))
        weights = (top * (1.0 / jnp.sum(top, axis=-1, keepdims=True))).astype(jnp.bfloat16)
        out_ref[rows, cut] = jnp.dot(
            weights, kv[:, width + h * head_dim : width + (h + 1) * head_dim],
            preferred_element_type=jnp.float32,
        ).astype(jnp.bfloat16)


def attend(query, kv, block_slot, scale):
    blocks_dev, per_block = block_slot.shape
    tokens, width = query.shape
    block_len = tokens // blocks_dev
    length, both = kv.shape[1:]
    heads = scale.shape[0]
    group = math.gcd(blocks_dev, ATTEND_BLOCKS)
    taken = group * per_block

    def part(j):
        return pl.BlockSpec((1, length, both), lambda b, slots: (slots[b * taken + j], 0, 0))

    return pl.pallas_call(
        functools.partial(attention_kernel, heads, group),
        out_shape=jax.ShapeDtypeStruct((tokens, width), jnp.bfloat16),
        grid_spec=pltpu.PrefetchScalarGridSpec(
            num_scalar_prefetch=1,
            grid=(blocks_dev // group,),
            in_specs=[
                pl.BlockSpec(memory_space=pltpu.SMEM),
                pl.BlockSpec((group * block_len, width), lambda b, slots: (b, 0)),
            ] + [part(j) for j in range(taken)],
            out_specs=pl.BlockSpec((group * block_len, width), lambda b, slots: (b, 0)),
        ),
        cost_estimate=pl.CostEstimate(
            flops=4 * tokens * per_block * length * width, bytes_accessed=4 * 2**20, transcendentals=0
        ),
    )(block_slot.reshape(-1), scale, query, *([kv] * taken))


def body(
    hidden,
    norm_gain,
    store,
    store_gain,
    passage_ids,
    w_pool,
    pool_mix,
    w_branch,
    w_query,
    w_key,
    w_value,
    sharpness,
    w_out,
    w_gate,
):
    holders = lax.axis_size("st")
    core = lax.axis_index("tp")
    flat_ids = passage_ids.reshape(-1)
    reads = flat_ids.shape[0]
    pass_dev, length, width = store.shape
    owner = lax.div(flat_ids, pass_dev)
    local = flat_ids - owner * pass_dev
    order = jnp.arange(reads, dtype=jnp.int32)
    earlier = (owner[None, :] == owner[:, None]) & (order[None, :] < order[:, None])
    rank = jnp.sum(earlier.astype(jnp.int32), axis=1)
    most = max(1, 2 * reads // holders)
    wanted = owner * most + rank
    hits = wanted[None, :] == jnp.arange(holders * most, dtype=jnp.int32)[:, None]
    request = jnp.sum(jnp.where(hits, local[None, :], 0), axis=1).reshape(holders, most)
    incoming = lax.all_to_all(request, "st", split_axis=0, concat_axis=0, tiled=True)

    passage_normed = rms_norm(store, store_gain).astype(jnp.bfloat16).reshape(pass_dev * length, width)
    w_kv = jnp.concatenate([w_key, w_value], axis=1)
    own_kv = jnp.dot(passage_normed, w_kv, preferred_element_type=jnp.float32).astype(jnp.bfloat16)
    own_kv = own_kv.reshape(pass_dev, length, -1)
    packed = own_kv[incoming.reshape(-1)]
    packed, hidden, w_out, w_branch = lax.optimization_barrier((packed, hidden, w_out, w_branch))
    kv = lax.all_to_all(packed, "st", split_axis=0, concat_axis=0, tiled=True)
    slot = wanted

    w_out_other = swap(columns_of(w_out, 1 - core))
    w_branch_other = swap(columns_of(w_branch, 1 - core))
    normed = rms_norm(hidden, norm_gain).astype(jnp.bfloat16)
    pool_out = pool_branch(normed, w_pool, pool_mix)
    branch_pool = half_terms(pool_out, swap(pool_out), columns_of(w_branch, core), w_branch_other)
    gate = jax.nn.sigmoid(jnp.dot(normed, w_gate, preferred_element_type=jnp.float32))
    query = jnp.dot(normed, w_query, preferred_element_type=jnp.float32).astype(jnp.bfloat16)

    head_dim = query.shape[1] // sharpness.shape[0]
    read = attend(query, kv, slot.reshape(passage_ids.shape), sharpness / math.sqrt(head_dim))
    branch_read = half_terms(read, swap(read), columns_of(w_out, core), w_out_other)
    return (branch_pool + gate * branch_read).astype(jnp.bfloat16)


def solution(mesh):
    placed = (
        P("st", None),
        P(),
        P("st", None, None),
        P(),
        P("st", None),
        P(None, "tp"),
        P("tp", None, None),
        P("tp", None),
        P(None, "tp"),
        P(None, "tp"),
        P(None, "tp"),
        P("tp"),
        P("tp", None),
        P(None, "tp"),
    )
    return jax.shard_map(body, mesh=mesh, in_specs=placed, out_specs=P("st", "tp"), check_vma=False)
```

```python
import functools
import math

import jax
import jax.numpy as jnp
from jax import lax
from jax.experimental import pallas as pl
from jax.experimental.pallas import tpu as pltpu
from jax.sharding import PartitionSpec as P

GROUPS = 4
ATTEND_BLOCKS = 8
MESH = pl.DeviceIdType.MESH


def rms_norm(values, gain):
    wide = values.astype(jnp.float32)
    scale = lax.rsqrt(jnp.mean(wide * wide, axis=-1, keepdims=True) + 1e-05)
    return wide * scale * gain


def pool_branch(normed, w_pool, pool_mix):
    tokens = normed.shape[0]
    local_groups = pool_mix.shape[0]
    group_dim = pool_mix.shape[1]
    pool_in = jnp.dot(normed, w_pool, preferred_element_type=jnp.float32).astype(jnp.bfloat16)
    grouped = pool_in.astype(jnp.float32).reshape(tokens, local_groups, group_dim)
    group_index = lax.axis_index("tp") * local_groups + jnp.arange(local_groups, dtype=jnp.int32)
    window = jnp.power(2, group_index + 1)
    total = jnp.zeros_like(grouped)
    for shift in range(2**GROUPS):
        shifted = jnp.pad(grouped, ((shift, 0), (0, 0), (0, 0)))[:tokens]
        total = total + jnp.where(shift < window, 1.0, 0.0)[None, :, None] * shifted
    position = jnp.arange(tokens, dtype=jnp.int32)[:, None]
    count = jnp.minimum(position + 1, window[None, :]).astype(jnp.float32)
    pooled = (total / count[:, :, None] - grouped).astype(jnp.bfloat16)
    pool_out = jnp.einsum("tgc,gcd->tgd", pooled, pool_mix, preferred_element_type=jnp.float32)
    return pool_out.astype(jnp.bfloat16).reshape(tokens, local_groups * group_dim)


def half_terms(own, other, weight_own, weight_other):
    terms = [
        jnp.dot(a, w, preferred_element_type=jnp.float32).astype(jnp.bfloat16).astype(jnp.float32)
        for a, w in ((own, weight_own), (other, weight_other))
    ]
    return terms[0] + terms[1]


def swap(array):
    return lax.ppermute(array, "tp", [(0, 1), (1, 0)])


def columns_of(weight, part):
    half = weight.shape[1] // 2
    return lax.dynamic_slice_in_dim(weight, part * half, half, axis=1)


def attention_kernel(heads, group, slots_ref, scale_ref, q_ref, *refs):
    parts, out_ref = refs[:-1], refs[-1]
    width = q_ref.shape[1]
    head_dim = width // heads
    block_len = q_ref.shape[0] // group
    per_block = len(parts) // group
    for b, h in [(b, h) for b in range(group) for h in range(heads)]:
        rows = slice(b * block_len, (b + 1) * block_len)
        kv = jnp.concatenate([r[0] for r in parts[b * per_block : (b + 1) * per_block]], axis=0)
        cut = slice(h * head_dim, (h + 1) * head_dim)
        scores = lax.dot_general(
            q_ref[rows, cut], kv[:, cut], (((1,), (1,)), ((), ())), preferred_element_type=jnp.float32
        )
        scores = scores * scale_ref[h]
        top = jnp.exp(scores - jnp.max(scores, axis=-1, keepdims=True))
        weights = (top * (1.0 / jnp.sum(top, axis=-1, keepdims=True))).astype(jnp.bfloat16)
        out_ref[rows, cut] = jnp.dot(
            weights, kv[:, width + h * head_dim : width + (h + 1) * head_dim],
            preferred_element_type=jnp.float32,
        ).astype(jnp.bfloat16)


def attend(query, kv, block_slot, scale):
    blocks_dev, per_block = block_slot.shape
    tokens, width = query.shape
    block_len = tokens // blocks_dev
    length, both = kv.shape[1:]
    heads = scale.shape[0]
    group = math.gcd(blocks_dev, ATTEND_BLOCKS)
    taken = group * per_block

    def part(j):
        return pl.BlockSpec((1, length, both), lambda b, slots: (slots[b * taken + j], 0, 0))

    return pl.pallas_call(
        functools.partial(attention_kernel, heads, group),
        out_shape=jax.ShapeDtypeStruct((tokens, width), jnp.bfloat16),
        grid_spec=pltpu.PrefetchScalarGridSpec(
            num_scalar_prefetch=1,
            grid=(blocks_dev // group,),
            in_specs=[
                pl.BlockSpec(memory_space=pltpu.SMEM),
                pl.BlockSpec((group * block_len, width), lambda b, slots: (b, 0)),
            ] + [part(j) for j in range(taken)],
            out_specs=pl.BlockSpec((group * block_len, width), lambda b, slots: (b, 0)),
        ),
        cost_estimate=pl.CostEstimate(
            flops=4 * tokens * per_block * length * width, bytes_accessed=4 * 2**20, transcendentals=0
        ),
    )(block_slot.reshape(-1), scale, query, *([kv] * taken))


def body(
    hidden,
    norm_gain,
    store,
    store_gain,
    passage_ids,
    w_pool,
    pool_mix,
    w_branch,
    w_query,
    w_key,
    w_value,
    sharpness,
    w_out,
    w_gate,
):
    holders = lax.axis_size("st")
    core = lax.axis_index("tp")
    flat_ids = passage_ids.reshape(-1)
    reads = flat_ids.shape[0]
    pass_dev, length, width = store.shape
    owner = lax.div(flat_ids, pass_dev)
    local = flat_ids - owner * pass_dev
    order = jnp.arange(reads, dtype=jnp.int32)
    earlier = (owner[None, :] == owner[:, None]) & (order[None, :] < order[:, None])
    rank = jnp.sum(earlier.astype(jnp.int32), axis=1)
    most = max(1, 2 * reads // holders)
    wanted = owner * most + rank
    hits = wanted[None, :] == jnp.arange(holders * most, dtype=jnp.int32)[:, None]
    request = jnp.sum(jnp.where(hits, local[None, :], 0), axis=1).reshape(holders, most)
    incoming = lax.all_to_all(request, "st", split_axis=0, concat_axis=0, tiled=True)

    passage_normed = rms_norm(store, store_gain).astype(jnp.bfloat16).reshape(pass_dev * length, width)
    w_kv = jnp.concatenate([w_key, w_value], axis=1)
    own_kv = jnp.dot(passage_normed, w_kv, preferred_element_type=jnp.float32).astype(jnp.bfloat16)
    own_kv = own_kv.reshape(pass_dev, length, -1)
    packed = own_kv[incoming.reshape(-1)]
    packed, hidden, w_out, w_branch = lax.optimization_barrier((packed, hidden, w_out, w_branch))
    kv = lax.all_to_all(packed, "st", split_axis=0, concat_axis=0, tiled=True)
    slot = wanted

    w_out_other = swap(columns_of(w_out, 1 - core))
    w_branch_other = swap(columns_of(w_branch, 1 - core))
    normed = rms_norm(hidden, norm_gain).astype(jnp.bfloat16)
    pool_out = pool_branch(normed, w_pool, pool_mix)
    branch_pool = half_terms(pool_out, swap(pool_out), columns_of(w_branch, core), w_branch_other)
    gate = jax.nn.sigmoid(jnp.dot(normed, w_gate, preferred_element_type=jnp.float32))
    query = jnp.dot(normed, w_query, preferred_element_type=jnp.float32).astype(jnp.bfloat16)

    head_dim = query.shape[1] // sharpness.shape[0]
    read = attend(query, kv, slot.reshape(passage_ids.shape), sharpness / math.sqrt(head_dim))
    branch_read = half_terms(read, swap(read), columns_of(w_out, core), w_out_other)
    return (branch_pool + gate * branch_read).astype(jnp.bfloat16)


def solution(mesh):
    placed = (
        P("st", None),
        P(),
        P("st", None, None),
        P(),
        P("st", None),
        P(None, "tp"),
        P("tp", None, None),
        P("tp", None),
        P(None, "tp"),
        P(None, "tp"),
        P(None, "tp"),
        P("tp"),
        P("tp", None),
        P(None, "tp"),
    )
    return jax.shard_map(body, mesh=mesh, in_specs=placed, out_specs=P("st", "tp"), check_vma=False)
```
